32 devices in a mesh: grp: 2 (over y), fs: 4 (over z), tp: 4 (over x, core).
Axes of the slice: x: 2, y: 2, z: 4, core: 2. Of those that a mesh axis runs over, the one named last changes fastest.
Arguments:
- tokens: bfloat16 [2048, 2048], P(('grp', 'fs'), 'tp'), parts along dimension 0, may hold values from -6 to 6
- recurrent_norm_gain: float32 [2048], replicated, may hold values from 0.1 to 1.9
- feedforward_norm_gain: float32 [2048], replicated, may hold values from 0.1 to 1.9
- gate_projection_weight: bfloat16 [2048, 2048], P('fs', 'tp'), may hold values from -0.125 to 0.125
- recurrent_projection_weight: bfloat16 [2048, 2048], P('fs', 'tp'), may hold values from -0.125 to 0.125
- convolution_kernel: bfloat16 [4, 2048], P(None, 'tp'), may hold values from -3 to 3
- decay_gate_matrix: bfloat16 [16, 128, 128], P('tp'), may hold values from -0.5 to 0.5
- input_gate_matrix: bfloat16 [16, 128, 128], P('tp'), may hold values from -0.5 to 0.5
- base_decay_logit: float32 [2048], P('tp'), may hold values from 3 to 9
- extra_log_decay: float32 [2048], P(('grp', 'fs')), parts along dimension 0, may hold values from -0.7 to 0
- output_projection_weight: bfloat16 [2048, 2048], P('tp', 'fs'), may hold values from -0.125 to 0.125
- up_projection_weight: bfloat16 [2048, 8192], P('fs', 'tp'), may hold values from -0.125 to 0.125
- down_projection_weight: bfloat16 [8192, 2048], P('tp', 'fs'), may hold values from -0.0625 to 0.0625
Outputs:
- layer_out: bfloat16 [2048, 2048], P(('grp', 'fs'), 'tp'), parts along dimension 0
The draws below stay inside these ranges and needn't reach their ends.
There are 2 independent parts, one for each index of `grp`. The reference program is written for one: setup_inputs(seed, part) draws one part's arguments, and reference() takes and returns one part's arrays. A program takes and returns all parts, laid end to end along the dimension named above; an argument that names none is the same for every part. Nothing has to cross between parts.
All inputs are finite; a program needn't handle non-finite values.
Results may differ from the reference program's by a relative error of at most 0.018.
Values may be sent and summed in bfloat16 or wider, within the bound.
A program may use at most 64 MiB of HBM per device.

```python
import math
import jax
import jax.numpy as jnp
from jax import lax

D = 2048
FF = 8192
BLOCKS = 16
BLOCK_DIM = 128
CONV = 4
SEQUENCE_TOKENS = 256
WIDTH = 2048
TOKENS = 1024
N_TP = 4


def draw_base_decay_logit(key, part):
    key_pick, key_slow, key_fast = jax.random.split(key, 3)
    share = 0.5
    chosen = jax.random.uniform(key_pick, (WIDTH,), jnp.float32) < share
    slow_rate = jnp.exp(jax.random.uniform(key_slow, (WIDTH,), jnp.float32, math.log(0.3), math.log(1.5))) / (4.0 * SEQUENCE_TOKENS)
    fast_rate = 0.25 / jnp.exp(jax.random.uniform(key_fast, (WIDTH,), jnp.float32, math.log(8.0), math.log(25.0)))
    decay_rate = jnp.where(chosen, fast_rate, slow_rate)
    return (-decay_rate - jnp.log(-jnp.expm1(-decay_rate))).astype(jnp.float32)


def draw_extra_log_decay(key, part):
    key_pick, key_depth = jax.random.split(key)
    picked = jax.random.randint(key_pick, (TOKENS,), 0, SEQUENCE_TOKENS) < 3
    depth = jnp.log(jax.random.uniform(key_depth, (TOKENS,), jnp.float32, 0.5, 0.8))
    return jnp.where(picked, depth, 0.0).astype(jnp.float32)


def block_levels(stream_key, shape, cuts, low, largest):
    gain, own = 1.0, jax.random.fold_in(stream_key, 6)
    for axis_at, shards_of in cuts:
        steps = jnp.exp(jax.random.uniform(jax.random.fold_in(own, axis_at), (shards_of,), jnp.float32, low / len(cuts), largest / len(cuts)))
        gain = gain * jnp.repeat(steps, shape[axis_at] // shards_of).reshape([-1 if axis == axis_at else 1 for axis in range(len(shape))])
    return gain


def noise(rng, shape, spread, bound, pieces=(), dtype=jnp.bfloat16):
    drawn = spread * jax.random.normal(rng, shape, jnp.float32)
    if pieces:
        drawn = drawn * block_levels(rng, shape, pieces, -0.22, 0.18)
    return jnp.clip(drawn, -bound, bound).astype(dtype)


def setup_inputs(seed: int = 0, part: int = 0) -> dict:
    key_list = jax.random.split(jax.random.key(seed), 14)
    part_keys = jax.random.split(jax.random.fold_in(key_list[13], part), 14)
    tokens = noise(part_keys[0], (TOKENS, D), 1.0, 6.0, ((0, 4), (1, 4)))
    recurrent_norm_gain = jnp.clip(1.0 + 0.18 * jax.random.normal(key_list[1], (D,), jnp.float32), 0.1, 1.9)
    feedforward_norm_gain = jnp.clip(1.0 + 0.18 * jax.random.normal(key_list[2], (D,), jnp.float32), 0.1, 1.9)
    gate_projection_weight = noise(key_list[3], (D, WIDTH), D ** -0.5, 0.125, ((0, 4), (1, 4)))
    recurrent_projection_weight = noise(key_list[4], (D, WIDTH), D ** -0.5, 0.125, ((0, 4), (1, 4)))
    convolution_kernel = noise(key_list[5], (CONV, WIDTH), 0.5, 3.0, ((1, 4),))
    decay_gate_matrix = noise(key_list[6], (BLOCKS, BLOCK_DIM, BLOCK_DIM), BLOCK_DIM ** -0.5, 0.5, ((0, 4),))
    input_gate_matrix = noise(key_list[7], (BLOCKS, BLOCK_DIM, BLOCK_DIM), BLOCK_DIM ** -0.5, 0.5, ((0, 4),))
    base_decay_logit = draw_base_decay_logit(jax.random.fold_in(key_list[13], 71), part)
    extra_log_decay = draw_extra_log_decay(jax.random.fold_in(jax.random.fold_in(key_list[13], part), 71), part)
    output_projection_weight = noise(key_list[10], (WIDTH, D), WIDTH ** -0.5, 0.125, ((0, 4), (1, 4)))
    up_projection_weight = noise(key_list[11], (D, FF), D ** -0.5, 0.125, ((0, 4), (1, 4)))
    down_projection_weight = noise(key_list[12], (FF, D), FF ** -0.5, 0.0625, ((0, 4), (1, 4)))
    return dict(tokens=tokens, recurrent_norm_gain=recurrent_norm_gain, feedforward_norm_gain=feedforward_norm_gain, gate_projection_weight=gate_projection_weight, recurrent_projection_weight=recurrent_projection_weight, convolution_kernel=convolution_kernel, decay_gate_matrix=decay_gate_matrix, input_gate_matrix=input_gate_matrix, base_decay_logit=base_decay_logit, extra_log_decay=extra_log_decay, output_projection_weight=output_projection_weight, up_projection_weight=up_projection_weight, down_projection_weight=down_projection_weight)


def rms_rows(values_in, norm_gain):
    values = values_in.astype(jnp.float32)
    inverse = lax.rsqrt(lax.optimization_barrier(jnp.mean(values * values, axis=-1, keepdims=True)) + 1e-06)
    return (values * inverse * norm_gain.astype(jnp.float32)).astype(jnp.bfloat16)

def combine(earlier, later):
    return (earlier[0] * later[0], later[0] * earlier[1] + later[1])

def recurrent_state(recurrent_branch_rows, gate_branch_rows, convolution_kernel, decay_gate_matrix, input_gate_matrix, base_decay_logit, extra_log_decay):
    length = recurrent_branch_rows.shape[0]
    taps = convolution_kernel.shape[0]
    padded = jnp.pad(recurrent_branch_rows.astype(jnp.float32), ((taps - 1, 0), (0, 0)))
    conv_sum = jnp.zeros((length, recurrent_branch_rows.shape[1]), jnp.float32)
    for tap_index in range(taps):
        conv_sum = conv_sum + padded[tap_index:tap_index + length] * convolution_kernel[tap_index].astype(jnp.float32)
    conv_rows = conv_sum.astype(jnp.bfloat16)
    blocks = decay_gate_matrix.shape[0]
    blocked = conv_rows.reshape(length, blocks, -1).astype(jnp.float32)
    recurrence_gate = jax.nn.sigmoid(jnp.einsum('tni,nij->tnj', blocked, decay_gate_matrix.astype(jnp.float32)).reshape(length, -1))
    input_rate = jax.nn.sigmoid(jnp.einsum('tni,nij->tnj', blocked, input_gate_matrix.astype(jnp.float32)).reshape(length, -1))
    decay_log_values = -8.0 * jax.nn.softplus(-base_decay_logit) * recurrence_gate + extra_log_decay[:, None]
    decay = jnp.exp(decay_log_values)
    drive = jnp.sqrt(-jnp.expm1(2.0 * decay_log_values)) * input_rate * conv_rows.astype(jnp.float32)
    _, hidden = lax.associative_scan(combine, (decay, drive), axis=0)
    return (hidden * gate_branch_rows.astype(jnp.float32)).astype(jnp.bfloat16)

def split_sum(left_rows, weight):
    block_width = weight.shape[0] // N_TP
    summed = jnp.zeros((left_rows.shape[0], weight.shape[1]), jnp.float32)
    for block_index in range(N_TP):
        lower = block_index * block_width
        partial_value = jnp.dot(left_rows[:, lower:lower + block_width], weight[lower:lower + block_width], preferred_element_type=jnp.float32).astype(jnp.bfloat16)
        summed = summed + lax.optimization_barrier(partial_value).astype(jnp.float32)
    return summed

def reference(tokens, recurrent_norm_gain, feedforward_norm_gain, gate_projection_weight, recurrent_projection_weight, convolution_kernel, decay_gate_matrix, input_gate_matrix, base_decay_logit, extra_log_decay, output_projection_weight, up_projection_weight, down_projection_weight):
    sequence_count = tokens.shape[0]
    sequence_batch = sequence_count // SEQUENCE_TOKENS
    normed = rms_rows(tokens, recurrent_norm_gain)
    gate_branch_rows = jax.nn.gelu(jnp.dot(normed, gate_projection_weight, preferred_element_type=jnp.float32)).astype(jnp.bfloat16)
    recurrent_branch_rows = jnp.dot(normed, recurrent_projection_weight, preferred_element_type=jnp.float32).astype(jnp.bfloat16)
    mixed_output = jax.vmap(recurrent_state, in_axes=(0, 0, None, None, None, None, 0))(recurrent_branch_rows.reshape(sequence_batch, SEQUENCE_TOKENS, -1), gate_branch_rows.reshape(sequence_batch, SEQUENCE_TOKENS, -1), convolution_kernel, decay_gate_matrix, input_gate_matrix, base_decay_logit, extra_log_decay.reshape(sequence_batch, SEQUENCE_TOKENS)).reshape(sequence_count, -1)
    residual = (tokens.astype(jnp.float32) + split_sum(mixed_output, output_projection_weight)).astype(jnp.bfloat16)
    channel_in = rms_rows(residual, feedforward_norm_gain)
    upward = jnp.maximum(jnp.dot(channel_in, up_projection_weight, preferred_element_type=jnp.float32), 0.0)
    squared = (upward * upward).astype(jnp.bfloat16)
    return (residual.astype(jnp.float32) + split_sum(squared, down_projection_weight)).astype(jnp.bfloat16)
```

```python
import jax
import jax.numpy as jnp
from jax import lax
from jax.sharding import PartitionSpec as P


def rms_rows(values_in, norm_gain):
    values = values_in.astype(jnp.float32)
    inverse = lax.rsqrt(jnp.mean(values * values, axis=-1, keepdims=True) + 1e-06)
    return (values * inverse * norm_gain).astype(jnp.bfloat16)


def combine(earlier, later):
    return (earlier[0] * later[0], later[0] * earlier[1] + later[1])


def recurrent_state(
    recurrent_branch_rows,
    gate_branch_rows,
    convolution_kernel,
    decay_gate_matrix,
    input_gate_matrix,
    base_decay_logit,
    extra_log_decay,
):
    length = recurrent_branch_rows.shape[0]
    taps = convolution_kernel.shape[0]
    padded = jnp.pad(recurrent_branch_rows.astype(jnp.float32), ((taps - 1, 0), (0, 0)))
    conv_sum = jnp.zeros((length, recurrent_branch_rows.shape[1]), jnp.float32)
    for tap_index in range(taps):
        conv_sum = conv_sum + padded[tap_index : tap_index + length] * convolution_kernel[
            tap_index
        ].astype(jnp.float32)
    conv_rows = conv_sum.astype(jnp.bfloat16)
    blocks = decay_gate_matrix.shape[0]
    blocked = conv_rows.reshape(length, blocks, -1)
    recurrence_gate = jax.nn.sigmoid(
        jnp.einsum(
            "tni,nij->tnj", blocked, decay_gate_matrix, preferred_element_type=jnp.float32
        ).reshape(length, -1)
    )
    input_rate = jax.nn.sigmoid(
        jnp.einsum(
            "tni,nij->tnj", blocked, input_gate_matrix, preferred_element_type=jnp.float32
        ).reshape(length, -1)
    )
    decay_log_values = (
        -8.0 * jax.nn.softplus(-base_decay_logit) * recurrence_gate + extra_log_decay[:, None]
    )
    decay = jnp.exp(decay_log_values)
    drive = (
        jnp.sqrt(-jnp.expm1(2.0 * decay_log_values)) * input_rate * conv_rows.astype(jnp.float32)
    )
    _, hidden = lax.associative_scan(combine, (decay, drive), axis=0)
    return (hidden * gate_branch_rows.astype(jnp.float32)).astype(jnp.bfloat16)


def per_device(
    tokens,
    recurrent_norm_gain,
    feedforward_norm_gain,
    gate_projection_weight,
    recurrent_projection_weight,
    convolution_kernel,
    decay_gate_matrix,
    input_gate_matrix,
    base_decay_logit,
    extra_log_decay,
    output_projection_weight,
    up_projection_weight,
    down_projection_weight,
):
    whole_rows = lax.all_gather(tokens, "tp", axis=1, tiled=True)
    normed = rms_rows(whole_rows, recurrent_norm_gain)
    columns = normed
    gate_pre = jnp.dot(
        columns,
        lax.all_gather(gate_projection_weight, "fs", axis=0, tiled=True),
        preferred_element_type=jnp.float32,
    )
    recur_pre = jnp.dot(
        columns,
        lax.all_gather(recurrent_projection_weight, "fs", axis=0, tiled=True),
        preferred_element_type=jnp.float32,
    )
    gate_branch_rows = jax.nn.gelu(gate_pre).astype(jnp.bfloat16)
    recurrent_branch_rows = recur_pre.astype(jnp.bfloat16)
    mixed_output = recurrent_state(
        recurrent_branch_rows,
        gate_branch_rows,
        convolution_kernel,
        decay_gate_matrix,
        input_gate_matrix,
        base_decay_logit,
        extra_log_decay,
    )
    partials = jnp.dot(
        mixed_output,
        lax.all_gather(output_projection_weight, "fs", axis=1, tiled=True),
        preferred_element_type=jnp.float32,
    )
    residual = (
        tokens.astype(jnp.float32)
        + lax.psum_scatter(
            partials.astype(jnp.bfloat16), "tp", scatter_dimension=1, tiled=True
        ).astype(jnp.float32)
    ).astype(jnp.bfloat16)
    middle = lax.all_gather(residual, "tp", axis=1, tiled=True)
    channel_in = rms_rows(middle, feedforward_norm_gain)
    columns = channel_in
    upward = jnp.dot(
        columns,
        lax.all_gather(up_projection_weight, "fs", axis=0, tiled=True),
        preferred_element_type=jnp.float32,
    )
    positive = jnp.maximum(upward, 0.0)
    squared = (positive * positive).astype(jnp.bfloat16)
    down_terms = jnp.dot(
        squared,
        lax.all_gather(down_projection_weight, "fs", axis=1, tiled=True),
        preferred_element_type=jnp.float32,
    )
    summed_down = lax.psum_scatter(
        down_terms.astype(jnp.bfloat16), "tp", scatter_dimension=1, tiled=True
    ).astype(jnp.float32)
    return (residual.astype(jnp.float32) + summed_down).astype(jnp.bfloat16)


def exchange_blocks(weight, split_axis, join_axis):
    count, mine = lax.axis_size("fs"), lax.axis_index("fs")
    planes, plane = lax.axis_size("grp"), lax.axis_index("grp")
    width = weight.shape[split_axis] // count
    depth = weight.shape[join_axis]

    def piece(owner):
        return lax.dynamic_slice_in_dim(weight, owner * width, width, split_axis)

    shape = list(weight.shape)
    shape[split_axis] = width
    shape[join_axis] = depth * count
    joined = jnp.zeros(shape, weight.dtype)

    def put(joined, value, row, column):
        place = [0, 0]
        place[join_axis] += column
        place[0] = place[0] + row
        return lax.dynamic_update_slice(joined, value, place)

    joined = put(joined, piece(mine), 0, mine * depth)
    share = (depth if join_axis == 0 else width) // planes
    for step in range(1, count):
        target = lax.rem(mine + step, count)
        source = lax.rem(mine - step + count, count)
        part = lax.dynamic_slice_in_dim(piece(target), plane * share, share, 0)
        part = lax.ppermute(part, "fs", [(i, (i + step) % count) for i in range(count)])
        joined = put(joined, part, plane * share, source * depth)
        for turn in range(1, planes):
            other = lax.ppermute(part, "grp", [(i, (i + turn) % planes) for i in range(planes)])
            origin = lax.rem(plane - turn + planes, planes)
            joined = put(joined, other, origin * share, source * depth)
    return joined


def gather_all(rows):
    rows = lax.all_gather(rows, "fs", axis=0, tiled=True)
    return lax.all_gather(rows, "tp", axis=1, tiled=True)


def scatter_sum(partials):
    partials = lax.psum_scatter(partials, "tp", scatter_dimension=1, tiled=True)
    return lax.psum_scatter(partials, "fs", scatter_dimension=0, tiled=True)


def per_device_owned(
    tokens,
    recurrent_norm_gain,
    feedforward_norm_gain,
    gate_projection_weight,
    recurrent_projection_weight,
    convolution_kernel,
    decay_gate_matrix,
    input_gate_matrix,
    base_decay_logit,
    extra_log_decay,
    output_projection_weight,
    up_projection_weight,
    down_projection_weight,
):
    count, mine = lax.axis_size("fs"), lax.axis_index("fs")
    length = tokens.shape[0]

    def own(value, axis):
        width = value.shape[axis] // count
        return lax.dynamic_slice_in_dim(value, mine * width, width, axis)

    gate_weight = exchange_blocks(gate_projection_weight, 1, 0)
    recur_weight = exchange_blocks(recurrent_projection_weight, 1, 0)
    out_weight = exchange_blocks(output_projection_weight, 0, 1)
    up_weight = exchange_blocks(up_projection_weight, 1, 0)
    down_weight = exchange_blocks(down_projection_weight, 0, 1)
    extra = lax.all_gather(extra_log_decay, "fs", axis=0, tiled=True)

    normed = rms_rows(gather_all(tokens), recurrent_norm_gain)
    gate_rows = jax.nn.gelu(
        jnp.dot(normed, gate_weight, preferred_element_type=jnp.float32)
    ).astype(jnp.bfloat16)
    recur_rows = jnp.dot(normed, recur_weight, preferred_element_type=jnp.float32).astype(
        jnp.bfloat16
    )
    mixed = jax.vmap(recurrent_state, in_axes=(0, 0, None, None, None, None, 0))(
        recur_rows.reshape(count, length, -1),
        gate_rows.reshape(count, length, -1),
        own(convolution_kernel, 1),
        own(decay_gate_matrix, 0),
        own(input_gate_matrix, 0),
        own(base_decay_logit, 0),
        extra.reshape(count, length),
    ).reshape(count * length, -1)
    partials = jnp.dot(mixed, out_weight, preferred_element_type=jnp.float32)
    summed = scatter_sum(partials.astype(jnp.bfloat16))
    residual = (tokens.astype(jnp.float32) + summed.astype(jnp.float32)).astype(jnp.bfloat16)
    channel_in = rms_rows(gather_all(residual), feedforward_norm_gain)
    positive = jnp.maximum(
        jnp.dot(channel_in, up_weight, preferred_element_type=jnp.float32), 0.0
    )
    squared = (positive * positive).astype(jnp.bfloat16)
    down_terms = jnp.dot(squared, down_weight, preferred_element_type=jnp.float32)
    summed_down = scatter_sum(down_terms.astype(jnp.bfloat16)).astype(jnp.float32)
    return (residual.astype(jnp.float32) + summed_down).astype(jnp.bfloat16)


def solution(mesh):
    placed = (
        P(("grp", "fs"), "tp"),
        P(),
        P(),
        P("fs", "tp"),
        P("fs", "tp"),
        P(None, "tp"),
        P("tp", None, None),
        P("tp", None, None),
        P("tp"),
        P(("grp", "fs")),
        P("tp", "fs"),
        P("fs", "tp"),
        P("tp", "fs"),
    )
    owners = mesh.shape["fs"] * mesh.shape["tp"]

    def run(*arrays):
        owned = arrays[6].shape[0] % owners == 0
        body = per_device_owned if owned else per_device
        return jax.shard_map(
            body, mesh=mesh, in_specs=placed, out_specs=P(("grp", "fs"), "tp"), check_vma=False
        )(*arrays)

    return run
```

```python
import functools

import jax
import jax.numpy as jnp
from jax import lax
from jax.experimental import pallas as pl
from jax.experimental.pallas import tpu as pltpu
from jax.sharding import PartitionSpec as P

MESH = pl.DeviceIdType.MESH


def rms_rows(values_in, norm_gain):
    values = values_in.astype(jnp.float32)
    inverse = lax.rsqrt(jnp.mean(values * values, axis=-1, keepdims=True) + 1e-06)
    return (values * inverse * norm_gain).astype(jnp.bfloat16)


def combine(earlier, later):
    return (earlier[0] * later[0], later[0] * earlier[1] + later[1])


def recurrent_state(
    recurrent_branch_rows,
    gate_branch_rows,
    convolution_kernel,
    decay_gate_matrix,
    input_gate_matrix,
    base_decay_logit,
    extra_log_decay,
):
    length = recurrent_branch_rows.shape[0]
    taps = convolution_kernel.shape[0]
    padded = jnp.pad(recurrent_branch_rows.astype(jnp.float32), ((taps - 1, 0), (0, 0)))
    conv_sum = jnp.zeros((length, recurrent_branch_rows.shape[1]), jnp.float32)
    for tap_index in range(taps):
        conv_sum = conv_sum + padded[tap_index : tap_index + length] * convolution_kernel[
            tap_index
        ].astype(jnp.float32)
    conv_rows = conv_sum.astype(jnp.bfloat16)
    blocks = decay_gate_matrix.shape[0]
    blocked = conv_rows.reshape(length, blocks, -1)
    recurrence_gate = jax.nn.sigmoid(
        jnp.einsum(
            "tni,nij->tnj", blocked, decay_gate_matrix, preferred_element_type=jnp.float32
        ).reshape(length, -1)
    )
    input_rate = jax.nn.sigmoid(
        jnp.einsum(
            "tni,nij->tnj", blocked, input_gate_matrix, preferred_element_type=jnp.float32
        ).reshape(length, -1)
    )
    decay_log_values = (
        -8.0 * jax.nn.softplus(-base_decay_logit) * recurrence_gate + extra_log_decay[:, None]
    )
    decay = jnp.exp(decay_log_values)
    drive = (
        jnp.sqrt(-jnp.expm1(2.0 * decay_log_values)) * input_rate * conv_rows.astype(jnp.float32)
    )
    _, hidden = lax.associative_scan(combine, (decay, drive), axis=0)
    return (hidden * gate_branch_rows.astype(jnp.float32)).astype(jnp.bfloat16)


def per_device(
    tokens,
    recurrent_norm_gain,
    feedforward_norm_gain,
    gate_projection_weight,
    recurrent_projection_weight,
    convolution_kernel,
    decay_gate_matrix,
    input_gate_matrix,
    base_decay_logit,
    extra_log_decay,
    output_projection_weight,
    up_projection_weight,
    down_projection_weight,
):
    whole_rows = lax.all_gather(tokens, "tp", axis=1, tiled=True)
    normed = rms_rows(whole_rows, recurrent_norm_gain)
    columns = normed
    gate_pre = jnp.dot(
        columns,
        lax.all_gather(gate_projection_weight, "fs", axis=0, tiled=True),
        preferred_element_type=jnp.float32,
    )
    recur_pre = jnp.dot(
        columns,
        lax.all_gather(recurrent_projection_weight, "fs", axis=0, tiled=True),
        preferred_element_type=jnp.float32,
    )
    gate_branch_rows = jax.nn.gelu(gate_pre).astype(jnp.bfloat16)
    recurrent_branch_rows = recur_pre.astype(jnp.bfloat16)
    mixed_output = recurrent_state(
        recurrent_branch_rows,
        gate_branch_rows,
        convolution_kernel,
        decay_gate_matrix,
        input_gate_matrix,
        base_decay_logit,
        extra_log_decay,
    )
    partials = jnp.dot(
        mixed_output,
        lax.all_gather(output_projection_weight, "fs", axis=1, tiled=True),
        preferred_element_type=jnp.float32,
    )
    residual = (
        tokens.astype(jnp.float32)
        + lax.psum_scatter(
            partials.astype(jnp.bfloat16), "tp", scatter_dimension=1, tiled=True
        ).astype(jnp.float32)
    ).astype(jnp.bfloat16)
    middle = lax.all_gather(residual, "tp", axis=1, tiled=True)
    channel_in = rms_rows(middle, feedforward_norm_gain)
    columns = channel_in
    upward = jnp.dot(
        columns,
        lax.all_gather(up_projection_weight, "fs", axis=0, tiled=True),
        preferred_element_type=jnp.float32,
    )
    positive = jnp.maximum(upward, 0.0)
    squared = (positive * positive).astype(jnp.bfloat16)
    down_terms = jnp.dot(
        squared,
        lax.all_gather(down_projection_weight, "fs", axis=1, tiled=True),
        preferred_element_type=jnp.float32,
    )
    summed_down = lax.psum_scatter(
        down_terms.astype(jnp.bfloat16), "tp", scatter_dimension=1, tiled=True
    ).astype(jnp.float32)
    return (residual.astype(jnp.float32) + summed_down).astype(jnp.bfloat16)


def exchange_blocks(weight, split_axis, join_axis):
    count, mine = lax.axis_size("fs"), lax.axis_index("fs")
    planes, plane = lax.axis_size("grp"), lax.axis_index("grp")
    width = weight.shape[split_axis] // count
    depth = weight.shape[join_axis]

    def piece(owner):
        return lax.dynamic_slice_in_dim(weight, owner * width, width, split_axis)

    shape = list(weight.shape)
    shape[split_axis] = width
    shape[join_axis] = depth * count
    joined = jnp.zeros(shape, weight.dtype)

    def put(joined, value, row, column):
        place = [0, 0]
        place[join_axis] += column
        place[0] = place[0] + row
        return lax.dynamic_update_slice(joined, value, place)

    joined = put(joined, piece(mine), 0, mine * depth)
    share = (depth if join_axis == 0 else width) // planes
    for step in range(1, count):
        target = lax.rem(mine + step, count)
        source = lax.rem(mine - step + count, count)
        part = lax.dynamic_slice_in_dim(piece(target), plane * share, share, 0)
        part = lax.ppermute(part, "fs", [(i, (i + step) % count) for i in range(count)])
        joined = put(joined, part, plane * share, source * depth)
        for turn in range(1, planes):
            other = lax.ppermute(part, "grp", [(i, (i + turn) % planes) for i in range(planes)])
            origin = lax.rem(plane - turn + planes, planes)
            joined = put(joined, other, origin * share, source * depth)
    return joined


def steps_by_distance(count):
    return sorted(range(1, count), key=lambda step: (min(step, count - step), step))


def greet(count, place, row):
    barrier = pltpu.get_barrier_semaphore()
    peers = [{"fs": lax.rem(place + step, count)} for step in range(1, count)]
    peers += [{"tp": row ^ 1}, {"tp": row ^ 2}]
    for peer in peers:
        pl.semaphore_signal(barrier, inc=1, device_id=peer, device_id_type=MESH)
    pl.semaphore_wait(barrier, len(peers))


def gather_kernel(count, own_ref, gain_ref, out_ref, held, send_z, send_x, send_c, arrived):
    place, row = lax.axis_index("fs"), lax.axis_index("tp")
    across, beside, corner = row ^ 2, row ^ 1, row ^ 3
    length, width = own_ref.shape
    greet(count, place, row)

    def copy(source, at, send_sem, peer):
        return pltpu.make_async_remote_copy(
            src_ref=source,
            dst_ref=held.at[at[0], at[1]],
            send_sem=send_sem,
            recv_sem=arrived.at[at[0], at[1]],
            device_id=peer,
            device_id_type=MESH,
        )

    started = []

    def send(source, at, send_sem, peer):
        moving = copy(source, at, send_sem, peer)
        moving.start()
        started.append(moving)

    def wait(at):
        copy(held.at[at[0], at[1]], at, arrived.at[at[0], at[1]], {"tp": beside}).wait_recv()

    order = steps_by_distance(count)
    for step in order:
        send(own_ref, (place, row), send_z.at[step], {"fs": lax.rem(place + step, count)})
    send(own_ref, (place, row), send_x.at[0], {"tp": across})
    send(own_ref, (place, row), send_c.at[0, 0], {"tp": beside})
    held[place, row] = own_ref[...]
    for step in [0] + order:
        origin = lax.rem(place - step + count, count)
        if step:
            wait((origin, row))
            block = held.at[origin, row]
            send(block, (origin, row), send_x.at[step], {"tp": across})
            send(block, (origin, row), send_c.at[0, step], {"tp": beside})
        wait((origin, across))
        send(held.at[origin, across], (origin, across), send_c.at[1, step], {"tp": beside})
    tile = 64
    for step in [0] + order:
        origin = lax.rem(place - step + count, count)
        wait((origin, beside))
        wait((origin, corner))

        def normalise(index, carry):
            rows = pl.ds(pl.multiple_of(index * tile, tile), tile)
            parts = [held[origin, part, rows].astype(jnp.float32) for part in range(4)]
            total = sum(jnp.sum(part * part, axis=-1, keepdims=True) for part in parts)
            inverse = lax.rsqrt(total / (4 * width) + 1e-06)
            at = pl.ds(pl.multiple_of(origin * length + index * tile, tile), tile)
            for number, part in enumerate(parts):
                columns = pl.ds(number * width, width)
                out_ref[at, columns] = (part * inverse * gain_ref[:, columns]).astype(
                    out_ref.dtype
                )
            return carry

        lax.fori_loop(0, length // tile, normalise, 0)
    for moving in started:
        moving.wait_send()


def gather_normed(rows, norm_gain, number):
    count = lax.axis_size("fs")
    length, width = rows.shape
    vmem = pl.BlockSpec(memory_space=pltpu.VMEM)
    dma = pltpu.SemaphoreType.DMA
    return pl.pallas_call(
        functools.partial(gather_kernel, count),
        out_shape=jax.ShapeDtypeStruct((count * length, 4 * width), rows.dtype),
        in_specs=[vmem, vmem],
        out_specs=vmem,
        scratch_shapes=[
            pltpu.VMEM((count, 4, length, width), rows.dtype),
            dma((count,)),
            dma((count,)),
            dma((2, count)),
            dma((count, 4)),
        ],
        compiler_params=pltpu.CompilerParams(
            collective_id=number, has_side_effects=True, vmem_limit_bytes=24 * 2**20
        ),
        cost_estimate=pl.CostEstimate(flops=10**9, bytes_accessed=10**8, transcendentals=0),
    )(rows, norm_gain.reshape(1, -1))


def scatter_kernel(
    count, terms_ref, base_ref, out_ref,
    from_core, to_x, from_x, to_z, from_z, send_c, recv_c, send_x, recv_x, send_z, recv_z,
):
    place, row = lax.axis_index("fs"), lax.axis_index("tp")
    across, beside, corner = row ^ 2, row ^ 1, row ^ 3
    length, width = base_ref.shape
    greet(count, place, row)
    started = []

    def copy(source, target, send_sem, recv_sem, peer):
        return pltpu.make_async_remote_copy(
            src_ref=source,
            dst_ref=target,
            send_sem=send_sem,
            recv_sem=recv_sem,
            device_id=peer,
            device_id_type=MESH,
        )

    def send(*given):
        moving = copy(*given)
        moving.start()
        started.append(moving)

    def block(step, part):
        owner = lax.rem(place + step, count)
        return (
            pl.ds(pl.multiple_of(owner * length, length), length),
            pl.ds(pl.multiple_of(part * width, width), width),
        )

    def core_copy(step, side):
        part = corner if side else beside
        return (
            terms_ref.at[block(step, part)],
            from_core.at[side, step],
            send_c.at[side, step],
            recv_c.at[side, step],
            {"tp": beside},
        )

    def x_copy(step):
        return (to_x.at[step], from_x.at[step], send_x.at[step], recv_x.at[step], {"tp": across})

    def z_copy(step):
        peer = {"fs": lax.rem(place + step, count)}
        return (to_z.at[step], from_z.at[step], send_z.at[step], recv_z.at[step], peer)

    order = steps_by_distance(count)[::-1] + [0]
    for step in order:
        for side in (1, 0):
            send(*core_copy(step, side))
    wide = jnp.float32
    for step in order:
        copy(*core_copy(step, 1)).wait_recv()
        mine = terms_ref[block(step, across)].astype(wide)
        to_x[step] = (mine + from_core[1, step].astype(wide)).astype(to_x.dtype)
        send(*x_copy(step))
    total = base_ref[...].astype(wide)
    summed = None
    for step in order:
        copy(*core_copy(step, 0)).wait_recv()
        copy(*x_copy(step)).wait_recv()
        mine = terms_ref[block(step, row)].astype(wide) + from_core[0, step].astype(wide)
        mine = mine + from_x[step].astype(wide)
        if step:
            to_z[step] = mine.astype(to_z.dtype)
            send(*z_copy(step))
        else:
            summed = mine
    for step in order[:-1]:
        copy(*z_copy(step)).wait_recv()
        summed = summed + from_z[step].astype(wide)
    out_ref[...] = (total + summed).astype(out_ref.dtype)
    for moving in started:
        moving.wait_send()


def scatter_added(terms, base, number):
    count = lax.axis_size("fs")
    vmem = pl.BlockSpec(memory_space=pltpu.VMEM)
    dma = pltpu.SemaphoreType.DMA
    blocks = pltpu.VMEM((count,) + base.shape, base.dtype)
    return pl.pallas_call(
        functools.partial(scatter_kernel, count),
        out_shape=jax.ShapeDtypeStruct(base.shape, base.dtype),
        in_specs=[vmem, vmem],
        out_specs=vmem,
        scratch_shapes=[pltpu.VMEM((2, count) + base.shape, base.dtype)]
        + [blocks] * 4
        + [dma((2, count))] * 2
        + [dma((count,))] * 4,
        compiler_params=pltpu.CompilerParams(
            collective_id=number, has_side_effects=True, vmem_limit_bytes=24 * 2**20
        ),
        cost_estimate=pl.CostEstimate(flops=10**9, bytes_accessed=10**8, transcendentals=0),
    )(terms, base)


def recurrence_kernel(
    gate_ref, recur_ref, taps_ref, decay_map_ref, input_map_ref, rate_ref, extra_ref, out_ref
):
    wide = jnp.float32
    recur = recur_ref[...].astype(jnp.bfloat16).astype(wide)
    length = recur.shape[0]
    position = lax.broadcasted_iota(jnp.int32, recur.shape, 0)
    taps = taps_ref.shape[0]
    conv = recur * taps_ref[taps - 1 : taps].astype(wide)
    for tap in range(taps - 1):
        back = taps - 1 - tap
        earlier = jnp.where(position >= back, pltpu.roll(recur, back, 0), 0.0)
        conv = conv + earlier * taps_ref[tap : tap + 1].astype(wide)
    conv_rows = conv.astype(jnp.bfloat16)
    recur_gate = jax.nn.sigmoid(
        jnp.dot(conv_rows, decay_map_ref[0], preferred_element_type=wide)
    )
    input_rate = jax.nn.sigmoid(
        jnp.dot(conv_rows, input_map_ref[0], preferred_element_type=wide)
    )
    log_decay = rate_ref[...] * recur_gate + extra_ref[...]
    decay = jnp.exp(log_decay)
    spread = -jnp.tanh(log_decay) * (decay * decay + 1.0)
    drive = jnp.sqrt(spread) * input_rate * conv_rows.astype(wide)
    back = 1
    while back < length:
        inside = position >= back
        drive = drive + decay * jnp.where(inside, pltpu.roll(drive, back, 0), 0.0)
        if back * 2 < length:
            decay = decay * jnp.where(inside, pltpu.roll(decay, back, 0), 1.0)
        back *= 2
    gate_rows = jax.nn.gelu(gate_ref[...]).astype(jnp.bfloat16)
    out_ref[...] = (drive * gate_rows.astype(wide)).astype(out_ref.dtype)


def recurrence(both, taps, decay_map, input_map, rate, extra, count):
    blocks, size, _ = decay_map.shape
    length = both.shape[0] // count
    return pl.pallas_call(
        recurrence_kernel,
        grid=(count, blocks),
        out_shape=jax.ShapeDtypeStruct((count * length, blocks * size), jnp.bfloat16),
        in_specs=[
            pl.BlockSpec((length, size), lambda s, n: (s, n)),
            pl.BlockSpec((length, size), lambda s, n: (s, n + blocks)),
            pl.BlockSpec((taps.shape[0], size), lambda s, n: (0, n)),
            pl.BlockSpec((1, size, size), lambda s, n: (n, 0, 0)),
            pl.BlockSpec((1, size, size), lambda s, n: (n, 0, 0)),
            pl.BlockSpec((1, size), lambda s, n: (0, n)),
            pl.BlockSpec((length, 1), lambda s, n: (s, 0)),
        ],
        out_specs=pl.BlockSpec((length, size), lambda s, n: (s, n)),
        compiler_params=pltpu.CompilerParams(vmem_limit_bytes=24 * 2**20),
        cost_estimate=pl.CostEstimate(flops=10**8, bytes_accessed=10**7, transcendentals=10**6),
    )(both, both, taps, decay_map, input_map, rate.reshape(1, -1), extra.reshape(-1, 1))


def per_device_owned(
    tokens,
    recurrent_norm_gain,
    feedforward_norm_gain,
    gate_projection_weight,
    recurrent_projection_weight,
    convolution_kernel,
    decay_gate_matrix,
    input_gate_matrix,
    base_decay_logit,
    extra_log_decay,
    output_projection_weight,
    up_projection_weight,
    down_projection_weight,
):
    count, mine = lax.axis_size("fs"), lax.axis_index("fs")

    def own(value, axis):
        width = value.shape[axis] // count
        return lax.dynamic_slice_in_dim(value, mine * width, width, axis)

    depth = gate_projection_weight.shape[0]
    paired = [
        weight.reshape(depth, count, -1)
        for weight in (gate_projection_weight, recurrent_projection_weight)
    ]
    both_weight = exchange_blocks(jnp.concatenate(paired, axis=2).reshape(depth, -1), 1, 0)
    out_weight = exchange_blocks(output_projection_weight, 0, 1)
    up_weight = exchange_blocks(up_projection_weight, 1, 0)
    down_weight = exchange_blocks(down_projection_weight, 0, 1)
    extra = lax.all_gather(extra_log_decay, "fs", axis=0, tiled=True)

    normed = gather_normed(tokens, recurrent_norm_gain, 1)
    mixed = recurrence(
        jnp.dot(normed, both_weight, preferred_element_type=jnp.float32),
        own(convolution_kernel, 1),
        own(decay_gate_matrix, 0),
        own(input_gate_matrix, 0),
        -8.0 * jax.nn.softplus(-own(base_decay_logit, 0)),
        extra,
        count,
    )
    partials = jnp.dot(mixed, out_weight, preferred_element_type=jnp.float32)
    residual = scatter_added(partials.astype(jnp.bfloat16), tokens, 2)
    channel_in = gather_normed(residual, feedforward_norm_gain, 3)
    positive = jnp.maximum(
        jnp.dot(channel_in, up_weight, preferred_element_type=jnp.float32), 0.0
    )
    squared = (positive * positive).astype(jnp.bfloat16)
    down_terms = jnp.dot(squared, down_weight, preferred_element_type=jnp.float32)
    return scatter_added(down_terms.astype(jnp.bfloat16), residual, 4)


def solution(mesh):
    placed = (
        P(("grp", "fs"), "tp"),
        P(),
        P(),
        P("fs", "tp"),
        P("fs", "tp"),
        P(None, "tp"),
        P("tp", None, None),
        P("tp", None, None),
        P("tp"),
        P(("grp", "fs")),
        P("tp", "fs"),
        P("fs", "tp"),
        P("tp", "fs"),
    )
    owners = mesh.shape["fs"] * mesh.shape["tp"]

    def run(*arrays):
        owned = arrays[6].shape[0] % owners == 0 and mesh.shape["tp"] == 4
        body = per_device_owned if owned else per_device
        return jax.shard_map(
            body, mesh=mesh, in_specs=placed, out_specs=P(("grp", "fs"), "tp"), check_vma=False
        )(*arrays)

    return run
```

```python
import functools

import jax
import jax.numpy as jnp
from jax import lax
from jax.experimental import pallas as pl
from jax.experimental.pallas import tpu as pltpu
from jax.sharding import PartitionSpec as P

MESH = pl.DeviceIdType.MESH


def rms_rows(values_in, norm_gain):
    values = values_in.astype(jnp.float32)
    inverse = lax.rsqrt(jnp.mean(values * values, axis=-1, keepdims=True) + 1e-06)
    return (values * inverse * norm_gain).astype(jnp.bfloat16)


def combine(earlier, later):
    return (earlier[0] * later[0], later[0] * earlier[1] + later[1])


def recurrent_state(
    recurrent_branch_rows,
    gate_branch_rows,
    convolution_kernel,
    decay_gate_matrix,
    input_gate_matrix,
    base_decay_logit,
    extra_log_decay,
):
    length = recurrent_branch_rows.shape[0]
    taps = convolution_kernel.shape[0]
    padded = jnp.pad(recurrent_branch_rows.astype(jnp.float32), ((taps - 1, 0), (0, 0)))
    conv_sum = jnp.zeros((length, recurrent_branch_rows.shape[1]), jnp.float32)
    for tap_index in range(taps):
        conv_sum = conv_sum + padded[tap_index : tap_index + length] * convolution_kernel[
            tap_index
        ].astype(jnp.float32)
    conv_rows = conv_sum.astype(jnp.bfloat16)
    blocks = decay_gate_matrix.shape[0]
    blocked = conv_rows.reshape(length, blocks, -1)
    recurrence_gate = jax.nn.sigmoid(
        jnp.einsum(
            "tni,nij->tnj", blocked, decay_gate_matrix, preferred_element_type=jnp.float32
        ).reshape(length, -1)
    )
    input_rate = jax.nn.sigmoid(
        jnp.einsum(
            "tni,nij->tnj", blocked, input_gate_matrix, preferred_element_type=jnp.float32
        ).reshape(length, -1)
    )
    decay_log_values = (
        -8.0 * jax.nn.softplus(-base_decay_logit) * recurrence_gate + extra_log_decay[:, None]
    )
    decay = jnp.exp(decay_log_values)
    drive = (
        jnp.sqrt(-jnp.expm1(2.0 * decay_log_values)) * input_rate * conv_rows.astype(jnp.float32)
    )
    _, hidden = lax.associative_scan(combine, (decay, drive), axis=0)
    return (hidden * gate_branch_rows.astype(jnp.float32)).astype(jnp.bfloat16)


def per_device(
    tokens,
    recurrent_norm_gain,
    feedforward_norm_gain,
    gate_projection_weight,
    recurrent_projection_weight,
    convolution_kernel,
    decay_gate_matrix,
    input_gate_matrix,
    base_decay_logit,
    extra_log_decay,
    output_projection_weight,
    up_projection_weight,
    down_projection_weight,
):
    whole_rows = lax.all_gather(tokens, "tp", axis=1, tiled=True)
    normed = rms_rows(whole_rows, recurrent_norm_gain)
    columns = normed
    gate_pre = jnp.dot(
        columns,
        lax.all_gather(gate_projection_weight, "fs", axis=0, tiled=True),
        preferred_element_type=jnp.float32,
    )
    recur_pre = jnp.dot(
        columns,
        lax.all_gather(recurrent_projection_weight, "fs", axis=0, tiled=True),
        preferred_element_type=jnp.float32,
    )
    gate_branch_rows = jax.nn.gelu(gate_pre).astype(jnp.bfloat16)
    recurrent_branch_rows = recur_pre.astype(jnp.bfloat16)
    mixed_output = recurrent_state(
        recurrent_branch_rows,
        gate_branch_rows,
        convolution_kernel,
        decay_gate_matrix,
        input_gate_matrix,
        base_decay_logit,
        extra_log_decay,
    )
    partials = jnp.dot(
        mixed_output,
        lax.all_gather(output_projection_weight, "fs", axis=1, tiled=True),
        preferred_element_type=jnp.float32,
    )
    residual = (
        tokens.astype(jnp.float32)
        + lax.psum_scatter(
            partials.astype(jnp.bfloat16), "tp", scatter_dimension=1, tiled=True
        ).astype(jnp.float32)
    ).astype(jnp.bfloat16)
    middle = lax.all_gather(residual, "tp", axis=1, tiled=True)
    channel_in = rms_rows(middle, feedforward_norm_gain)
    columns = channel_in
    upward = jnp.dot(
        columns,
        lax.all_gather(up_projection_weight, "fs", axis=0, tiled=True),
        preferred_element_type=jnp.float32,
    )
    positive = jnp.maximum(upward, 0.0)
    squared = (positive * positive).astype(jnp.bfloat16)
    down_terms = jnp.dot(
        squared,
        lax.all_gather(down_projection_weight, "fs", axis=1, tiled=True),
        preferred_element_type=jnp.float32,
    )
    summed_down = lax.psum_scatter(
        down_terms.astype(jnp.bfloat16), "tp", scatter_dimension=1, tiled=True
    ).astype(jnp.float32)
    return (residual.astype(jnp.float32) + summed_down).astype(jnp.bfloat16)


def steps_by_distance(count):
    return sorted(range(1, count), key=lambda step: (min(step, count - step), step))


def greet(count, place, row):
    barrier = pltpu.get_barrier_semaphore()
    peers = [{"fs": lax.rem(place + step, count)} for step in range(1, count)]
    peers += [{"tp": row ^ 1}, {"tp": row ^ 2}, {"grp": 1 - lax.axis_index("grp")}]
    for peer in peers:
        pl.semaphore_signal(barrier, inc=1, device_id=peer, device_id_type=MESH)
    pl.semaphore_wait(barrier, len(peers))


class Exchange:
    def __init__(self, count, axis, weight, joined, sems):
        self.count, self.axis, self.weight, self.joined, self.sems = (
            count, axis, weight, joined, sems
        )
        self.place, self.plane = lax.axis_index("fs"), lax.axis_index("grp")
        self.width = weight.shape[axis] // count
        self.depth = weight.shape[1 - axis]
        self.share = (self.depth if axis else self.width) // 2
        self.order = steps_by_distance(count)
        self.started = []

    def spot(self, rows, columns, row_step, column_step):
        return (
            pl.ds(pl.multiple_of(rows, row_step), self.share),
            pl.ds(pl.multiple_of(columns, column_step), self.width if self.axis else self.depth),
        )

    def leaving(self, owner, plane):
        half = plane * self.share
        if self.axis:
            return self.spot(half, owner * self.width, self.share, self.width)
        return self.spot(owner * self.width + half, 0, self.share, self.depth)

    def landing(self, source, plane):
        half = plane * self.share
        if self.axis:
            return self.spot(source * self.depth + half, 0, self.share, self.width)
        return self.spot(half, source * self.depth, self.share, self.depth)

    def copy(self, source, target, stage, step, peer):
        return pltpu.make_async_remote_copy(
            src_ref=source,
            dst_ref=target,
            send_sem=self.sems.at[stage, step],
            recv_sem=self.sems.at[stage + 1, step],
            device_id=peer,
            device_id_type=MESH,
        )

    def begin(self):
        for step in self.order:
            owner = lax.rem(self.place + step, self.count)
            moving = self.copy(
                self.weight.at[self.leaving(owner, self.plane)],
                self.joined.at[self.landing(self.place, self.plane)],
                0, step, {"fs": owner},
            )
            moving.start()
            self.started.append(moving)
        for plane in range(2):
            self.joined[self.landing(self.place, plane)] = self.weight[
                self.leaving(self.place, plane)
            ]

    def forward(self, step):
        source = lax.rem(self.place - step + self.count, self.count)
        peer = {"grp": 1 - self.plane}
        here = self.joined.at[self.landing(source, self.plane)]
        self.copy(here, here, 0, step, peer).wait_recv()
        moving = self.copy(here, here, 2, step, peer)
        moving.start()
        self.started.append(moving)

    def finish(self):
        for step in self.order:
            source = lax.rem(self.place - step + self.count, self.count)
            there = self.joined.at[self.landing(source, 1 - self.plane)]
            self.copy(there, there, 2, step, {"grp": 1 - self.plane}).wait_recv()
        for moving in self.started:
            moving.wait_send()


def joined_shape(weight, axis, count):
    shape = list(weight.shape)
    shape[axis] //= count
    shape[1 - axis] *= count
    return jax.ShapeDtypeStruct(tuple(shape), weight.dtype)


def gather_kernel(count, axes, *refs):
    held, send_z, send_x, send_c, arrived, moves, extra_sems = refs[-7:]
    own_ref, gain_ref, extra_ref = refs[:3]
    number = len(axes)
    out_ref, extra_out = refs[3 + number : 5 + number]
    exchanges = [
        Exchange(count, axis, refs[3 + k], refs[5 + number + k], moves.at[k])
        for k, axis in enumerate(axes)
    ]
    place, row = lax.axis_index("fs"), lax.axis_index("tp")
    across, beside, corner = row ^ 2, row ^ 1, row ^ 3
    length, width = own_ref.shape
    greet(count, place, row)

    def copy(source, at, send_sem, peer):
        return pltpu.make_async_remote_copy(
            src_ref=source,
            dst_ref=held.at[at[0], at[1]],
            send_sem=send_sem,
            recv_sem=arrived.at[at[0], at[1]],
            device_id=peer,
            device_id_type=MESH,
        )

    started = []

    def send(source, at, send_sem, peer):
        moving = copy(source, at, send_sem, peer)
        moving.start()
        started.append(moving)

    def wait(at):
        copy(held.at[at[0], at[1]], at, arrived.at[at[0], at[1]], {"tp": beside}).wait_recv()

    order = steps_by_distance(count)
    for step in order:
        send(own_ref, (place, row), send_z.at[step], {"fs": lax.rem(place + step, count)})
    send(own_ref, (place, row), send_x.at[0], {"tp": across})
    send(own_ref, (place, row), send_c.at[0, 0], {"tp": beside})
    for step in order:
        peer = lax.rem(place + step, count)
        moving = pltpu.make_async_remote_copy(
            src_ref=extra_ref.at[0],
            dst_ref=extra_out.at[place],
            send_sem=extra_sems.at[0, step],
            recv_sem=extra_sems.at[1, step],
            device_id={"fs": peer},
            device_id_type=MESH,
        )
        moving.start()
        started.append(moving)
    extra_out[place] = extra_ref[0]
    for exchange in exchanges:
        exchange.begin()
    held[place, row] = own_ref[...]
    for step in [0] + order:
        origin = lax.rem(place - step + count, count)
        if step:
            wait((origin, row))
            block = held.at[origin, row]
            send(block, (origin, row), send_x.at[step], {"tp": across})
            send(block, (origin, row), send_c.at[0, step], {"tp": beside})
        wait((origin, across))
        send(held.at[origin, across], (origin, across), send_c.at[1, step], {"tp": beside})
    for exchange in exchanges:
        for step in order:
            exchange.forward(step)
    tile = 64
    for step in [0] + order:
        origin = lax.rem(place - step + count, count)
        wait((origin, beside))
        wait((origin, corner))

        def normalise(index, carry):
            rows = pl.ds(pl.multiple_of(index * tile, tile), tile)
            parts = [held[origin, part, rows].astype(jnp.float32) for part in range(4)]
            total = sum(jnp.sum(part * part, axis=-1, keepdims=True) for part in parts)
            inverse = lax.rsqrt(total / (4 * width) + 1e-06)
            at = pl.ds(pl.multiple_of(origin * length + index * tile, tile), tile)
            for number, part in enumerate(parts):
                columns = pl.ds(number * width, width)
                out_ref[at, columns] = (part * inverse * gain_ref[:, columns]).astype(
                    out_ref.dtype
                )
            return carry

        lax.fori_loop(0, length // tile, normalise, 0)
    for exchange in exchanges:
        exchange.finish()
    for step in order:
        there = extra_out.at[lax.rem(place - step + count, count)]
        pltpu.make_async_remote_copy(
            src_ref=there,
            dst_ref=there,
            send_sem=extra_sems.at[0, step],
            recv_sem=extra_sems.at[1, step],
            device_id={"tp": beside},
            device_id_type=MESH,
        ).wait_recv()
    for moving in started:
        moving.wait_send()


def gather_normed(rows, norm_gain, extra, weights, axes, number):
    count = lax.axis_size("fs")
    length, width = rows.shape
    vmem = pl.BlockSpec(memory_space=pltpu.VMEM)
    dma = pltpu.SemaphoreType.DMA
    return pl.pallas_call(
        functools.partial(gather_kernel, count, axes),
        out_shape=[
            jax.ShapeDtypeStruct((count * length, 4 * width), rows.dtype),
            jax.ShapeDtypeStruct((count, 1, length), extra.dtype),
        ]
        + [joined_shape(weight, axis, count) for weight, axis in zip(weights, axes)],
        in_specs=[vmem] * (3 + len(axes)),
        out_specs=[vmem] * (2 + len(axes)),
        scratch_shapes=[
            pltpu.VMEM((count, 4, length, width), rows.dtype),
            dma((count,)),
            dma((count,)),
            dma((2, count)),
            dma((count, 4)),
            dma((len(axes), 4, count)),
            dma((2, count)),
        ],
        compiler_params=pltpu.CompilerParams(
            collective_id=number, has_side_effects=True, vmem_limit_bytes=32 * 2**20
        ),
        cost_estimate=pl.CostEstimate(flops=10**9, bytes_accessed=10**8, transcendentals=0),
    )(rows, norm_gain.reshape(1, -1), extra.reshape(1, 1, -1), *weights)


def scatter_kernel(count, axes, *refs):
    number = len(axes)
    terms_ref, base_ref = refs[:2]
    out_ref = refs[2 + number]
    from_core, to_x, from_x, to_z, from_z, send_c, recv_c, send_x, recv_x, send_z, recv_z = refs[
        3 + 2 * number : 14 + 2 * number
    ]
    exchanges = [
        Exchange(count, axis, refs[2 + k], refs[3 + number + k], refs[-1].at[k])
        for k, axis in enumerate(axes)
    ]
    place, row = lax.axis_index("fs"), lax.axis_index("tp")
    across, beside, corner = row ^ 2, row ^ 1, row ^ 3
    length, width = base_ref.shape
    greet(count, place, row)
    started = []

    def copy(source, target, send_sem, recv_sem, peer):
        return pltpu.make_async_remote_copy(
            src_ref=source,
            dst_ref=target,
            send_sem=send_sem,
            recv_sem=recv_sem,
            device_id=peer,
            device_id_type=MESH,
        )

    def send(*given):
        moving = copy(*given)
        moving.start()
        started.append(moving)

    def block(step, part):
        owner = lax.rem(place + step, count)
        return (
            pl.ds(pl.multiple_of(owner * length, length), length),
            pl.ds(pl.multiple_of(part * width, width), width),
        )

    def core_copy(step, side):
        part = corner if side else beside
        return (
            terms_ref.at[block(step, part)],
            from_core.at[side, step],
            send_c.at[side, step],
            recv_c.at[side, step],
            {"tp": beside},
        )

    def x_copy(step):
        return (to_x.at[step], from_x.at[step], send_x.at[step], recv_x.at[step], {"tp": across})

    def z_copy(step):
        peer = {"fs": lax.rem(place + step, count)}
        return (to_z.at[step], from_z.at[step], send_z.at[step], recv_z.at[step], peer)

    order = steps_by_distance(count)[::-1] + [0]
    for step in order:
        for side in (1, 0):
            send(*core_copy(step, side))
    wide = jnp.float32
    for exchange in exchanges:
        exchange.begin()
    for step in order:
        copy(*core_copy(step, 1)).wait_recv()
        mine = terms_ref[block(step, across)].astype(wide)
        to_x[step] = (mine + from_core[1, step].astype(wide)).astype(to_x.dtype)
        send(*x_copy(step))
    total = base_ref[...].astype(wide)
    summed = None
    for turn, step in enumerate(order):
        if turn:
            for exchange in exchanges:
                exchange.forward(exchange.order[turn - 1])
        copy(*core_copy(step, 0)).wait_recv()
        copy(*x_copy(step)).wait_recv()
        mine = terms_ref[block(step, row)].astype(wide) + from_core[0, step].astype(wide)
        mine = mine + from_x[step].astype(wide)
        if step:
            to_z[step] = mine.astype(to_z.dtype)
            send(*z_copy(step))
        else:
            summed = mine
    for step in order[:-1]:
        copy(*z_copy(step)).wait_recv()
        summed = summed + from_z[step].astype(wide)
    out_ref[...] = (total + summed).astype(out_ref.dtype)
    for exchange in exchanges:
        exchange.finish()
    for moving in started:
        moving.wait_send()


def scatter_added(terms, base, weights, axes, number):
    count = lax.axis_size("fs")
    vmem = pl.BlockSpec(memory_space=pltpu.VMEM)
    dma = pltpu.SemaphoreType.DMA
    blocks = pltpu.VMEM((count,) + base.shape, base.dtype)
    return pl.pallas_call(
        functools.partial(scatter_kernel, count, axes),
        out_shape=[jax.ShapeDtypeStruct(base.shape, base.dtype)]
        + [joined_shape(weight, axis, count) for weight, axis in zip(weights, axes)],
        in_specs=[vmem] * (2 + len(axes)),
        out_specs=[vmem] * (1 + len(axes)),
        scratch_shapes=[pltpu.VMEM((2, count) + base.shape, base.dtype)]
        + [blocks] * 4
        + [dma((2, count))] * 2
        + [dma((count,))] * 4
        + [dma((len(axes), 4, count)) for _ in axes[:1]],
        compiler_params=pltpu.CompilerParams(
            collective_id=number, has_side_effects=True, vmem_limit_bytes=24 * 2**20
        ),
        cost_estimate=pl.CostEstimate(flops=10**9, bytes_accessed=10**8, transcendentals=0),
    )(terms, base, *weights)


def recurrence_kernel(
    gate_ref, recur_ref, taps_ref, decay_map_ref, input_map_ref, rate_ref, extra_ref, out_ref
):
    wide = jnp.float32
    recur = recur_ref[...].astype(jnp.bfloat16).astype(wide)
    length = recur.shape[0]
    position = lax.broadcasted_iota(jnp.int32, recur.shape, 0)
    taps = taps_ref.shape[0]
    conv = recur * taps_ref[taps - 1 : taps].astype(wide)
    for tap in range(taps - 1):
        back = taps - 1 - tap
        earlier = jnp.where(position >= back, pltpu.roll(recur, back, 0), 0.0)
        conv = conv + earlier * taps_ref[tap : tap + 1].astype(wide)
    conv_rows = conv.astype(jnp.bfloat16)
    recur_gate = jax.nn.sigmoid(
        jnp.dot(conv_rows, decay_map_ref[0], preferred_element_type=wide)
    )
    input_rate = jax.nn.sigmoid(
        jnp.dot(conv_rows, input_map_ref[0], preferred_element_type=wide)
    )
    log_decay = rate_ref[...] * recur_gate + extra_ref[...]
    decay = jnp.exp(log_decay)
    spread = -jnp.tanh(log_decay) * (decay * decay + 1.0)
    drive = jnp.sqrt(spread) * input_rate * conv_rows.astype(wide)
    back = 1
    while back < length:
        inside = position >= back
        drive = drive + decay * jnp.where(inside, pltpu.roll(drive, back, 0), 0.0)
        if back * 2 < length:
            decay = decay * jnp.where(inside, pltpu.roll(decay, back, 0), 1.0)
        back *= 2
    gate_rows = jax.nn.gelu(gate_ref[...]).astype(jnp.bfloat16)
    out_ref[...] = (drive * gate_rows.astype(wide)).astype(out_ref.dtype)


def recurrence(both, taps, decay_map, input_map, rate, extra, count):
    blocks, size, _ = decay_map.shape
    length = both.shape[0] // count
    return pl.pallas_call(
        recurrence_kernel,
        grid=(count, blocks),
        out_shape=jax.ShapeDtypeStruct((count * length, blocks * size), jnp.bfloat16),
        in_specs=[
            pl.BlockSpec((length, size), lambda s, n: (s, n)),
            pl.BlockSpec((length, size), lambda s, n: (s, n + blocks)),
            pl.BlockSpec((taps.shape[0], size), lambda s, n: (0, n)),
            pl.BlockSpec((1, size, size), lambda s, n: (n, 0, 0)),
            pl.BlockSpec((1, size, size), lambda s, n: (n, 0, 0)),
            pl.BlockSpec((1, size), lambda s, n: (0, n)),
            pl.BlockSpec((length, 1), lambda s, n: (s, 0)),
        ],
        out_specs=pl.BlockSpec((length, size), lambda s, n: (s, n)),
        compiler_params=pltpu.CompilerParams(vmem_limit_bytes=24 * 2**20),
        cost_estimate=pl.CostEstimate(flops=10**8, bytes_accessed=10**7, transcendentals=10**6),
    )(both, both, taps, decay_map, input_map, rate.reshape(1, -1), extra.reshape(-1, 1))


def per_device_owned(
    tokens,
    recurrent_norm_gain,
    feedforward_norm_gain,
    gate_projection_weight,
    recurrent_projection_weight,
    convolution_kernel,
    decay_gate_matrix,
    input_gate_matrix,
    base_decay_logit,
    extra_log_decay,
    output_projection_weight,
    up_projection_weight,
    down_projection_weight,
):
    count, mine = lax.axis_size("fs"), lax.axis_index("fs")

    def own(value, axis):
        width = value.shape[axis] // count
        return lax.dynamic_slice_in_dim(value, mine * width, width, axis)

    depth = gate_projection_weight.shape[0]
    paired = [
        weight.reshape(depth, count, -1)
        for weight in (gate_projection_weight, recurrent_projection_weight)
    ]
    paired = jnp.concatenate(paired, axis=2).reshape(depth, -1)
    normed, extra, both_weight, out_weight = gather_normed(
        tokens,
        recurrent_norm_gain,
        extra_log_decay,
        (paired, output_projection_weight),
        (1, 0),
        1,
    )
    mixed = recurrence(
        jnp.dot(normed, both_weight, preferred_element_type=jnp.float32),
        own(convolution_kernel, 1),
        own(decay_gate_matrix, 0),
        own(input_gate_matrix, 0),
        -8.0 * jax.nn.softplus(-own(base_decay_logit, 0)),
        extra,
        count,
    )
    partials = jnp.dot(mixed, out_weight, preferred_element_type=jnp.float32)
    residual, up_weight = scatter_added(
        partials.astype(jnp.bfloat16), tokens, (up_projection_weight,), (1,), 2
    )
    channel_in, _, down_weight = gather_normed(
        residual, feedforward_norm_gain, extra_log_decay, (down_projection_weight,), (0,), 3
    )
    positive = jnp.maximum(
        jnp.dot(channel_in, up_weight, preferred_element_type=jnp.float32), 0.0
    )
    squared = (positive * positive).astype(jnp.bfloat16)
    down_terms = jnp.dot(squared, down_weight, preferred_element_type=jnp.float32)
    return scatter_added(down_terms.astype(jnp.bfloat16), residual, (), (), 4)[0]


def solution(mesh):
    placed = (
        P(("grp", "fs"), "tp"),
        P(),
        P(),
        P("fs", "tp"),
        P("fs", "tp"),
        P(None, "tp"),
        P("tp", None, None),
        P("tp", None, None),
        P("tp"),
        P(("grp", "fs")),
        P("tp", "fs"),
        P("fs", "tp"),
        P("tp", "fs"),
    )
    owners = mesh.shape["fs"] * mesh.shape["tp"]
    fitting = mesh.shape["tp"] == 4 and mesh.shape["grp"] == 2

    def run(*arrays):
        owned = fitting and arrays[6].shape[0] % owners == 0
        body = per_device_owned if owned else per_device
        return jax.shard_map(
            body, mesh=mesh, in_specs=placed, out_specs=P(("grp", "fs"), "tp"), check_vma=False
        )(*arrays)

    return run
```

```python
import functools

import jax
import jax.numpy as jnp
from jax import lax
from jax.experimental import pallas as pl
from jax.experimental.pallas import tpu as pltpu
from jax.sharding import PartitionSpec as P

MESH = pl.DeviceIdType.MESH


def rms_rows(values_in, norm_gain):
    values = values_in.astype(jnp.float32)
    inverse = lax.rsqrt(jnp.mean(values * values, axis=-1, keepdims=True) + 1e-06)
    return (values * inverse * norm_gain).astype(jnp.bfloat16)


def combine(earlier, later):
    return (earlier[0] * later[0], later[0] * earlier[1] + later[1])


def recurrent_state(
    recurrent_branch_rows,
    gate_branch_rows,
    convolution_kernel,
    decay_gate_matrix,
    input_gate_matrix,
    base_decay_logit,
    extra_log_decay,
):
    length = recurrent_branch_rows.shape[0]
    taps = convolution_kernel.shape[0]
    padded = jnp.pad(recurrent_branch_rows.astype(jnp.float32), ((taps - 1, 0), (0, 0)))
    conv_sum = jnp.zeros((length, recurrent_branch_rows.shape[1]), jnp.float32)
    for tap_index in range(taps):
        conv_sum = conv_sum + padded[tap_index : tap_index + length] * convolution_kernel[
            tap_index
        ].astype(jnp.float32)
    conv_rows = conv_sum.astype(jnp.bfloat16)
    blocks = decay_gate_matrix.shape[0]
    blocked = conv_rows.reshape(length, blocks, -1)
    recurrence_gate = jax.nn.sigmoid(
        jnp.einsum(
            "tni,nij->tnj", blocked, decay_gate_matrix, preferred_element_type=jnp.float32
        ).reshape(length, -1)
    )
    input_rate = jax.nn.sigmoid(
        jnp.einsum(
            "tni,nij->tnj", blocked, input_gate_matrix, preferred_element_type=jnp.float32
        ).reshape(length, -1)
    )
    decay_log_values = (
        -8.0 * jax.nn.softplus(-base_decay_logit) * recurrence_gate + extra_log_decay[:, None]
    )
    decay = jnp.exp(decay_log_values)
    drive = (
        jnp.sqrt(-jnp.expm1(2.0 * decay_log_values)) * input_rate * conv_rows.astype(jnp.float32)
    )
    _, hidden = lax.associative_scan(combine, (decay, drive), axis=0)
    return (hidden * gate_branch_rows.astype(jnp.float32)).astype(jnp.bfloat16)


def per_device(
    tokens,
    recurrent_norm_gain,
    feedforward_norm_gain,
    gate_projection_weight,
    recurrent_projection_weight,
    convolution_kernel,
    decay_gate_matrix,
    input_gate_matrix,
    base_decay_logit,
    extra_log_decay,
    output_projection_weight,
    up_projection_weight,
    down_projection_weight,
):
    whole_rows = lax.all_gather(tokens, "tp", axis=1, tiled=True)
    normed = rms_rows(whole_rows, recurrent_norm_gain)
    columns = normed
    gate_pre = jnp.dot(
        columns,
        lax.all_gather(gate_projection_weight, "fs", axis=0, tiled=True),
        preferred_element_type=jnp.float32,
    )
    recur_pre = jnp.dot(
        columns,
        lax.all_gather(recurrent_projection_weight, "fs", axis=0, tiled=True),
        preferred_element_type=jnp.float32,
    )
    gate_branch_rows = jax.nn.gelu(gate_pre).astype(jnp.bfloat16)
    recurrent_branch_rows = recur_pre.astype(jnp.bfloat16)
    mixed_output = recurrent_state(
        recurrent_branch_rows,
        gate_branch_rows,
        convolution_kernel,
        decay_gate_matrix,
        input_gate_matrix,
        base_decay_logit,
        extra_log_decay,
    )
    partials = jnp.dot(
        mixed_output,
        lax.all_gather(output_projection_weight, "fs", axis=1, tiled=True),
        preferred_element_type=jnp.float32,
    )
    residual = (
        tokens.astype(jnp.float32)
        + lax.psum_scatter(
            partials.astype(jnp.bfloat16), "tp", scatter_dimension=1, tiled=True
        ).astype(jnp.float32)
    ).astype(jnp.bfloat16)
    middle = lax.all_gather(residual, "tp", axis=1, tiled=True)
    channel_in = rms_rows(middle, feedforward_norm_gain)
    columns = channel_in
    upward = jnp.dot(
        columns,
        lax.all_gather(up_projection_weight, "fs", axis=0, tiled=True),
        preferred_element_type=jnp.float32,
    )
    positive = jnp.maximum(upward, 0.0)
    squared = (positive * positive).astype(jnp.bfloat16)
    down_terms = jnp.dot(
        squared,
        lax.all_gather(down_projection_weight, "fs", axis=1, tiled=True),
        preferred_element_type=jnp.float32,
    )
    summed_down = lax.psum_scatter(
        down_terms.astype(jnp.bfloat16), "tp", scatter_dimension=1, tiled=True
    ).astype(jnp.float32)
    return (residual.astype(jnp.float32) + summed_down).astype(jnp.bfloat16)


def steps_by_distance(count):
    return sorted(range(1, count), key=lambda step: (min(step, count - step), step))


def greet(count, place, row):
    barrier = pltpu.get_barrier_semaphore()
    peers = [{"fs": lax.rem(place + step, count)} for step in range(1, count)]
    peers += [{"tp": row ^ 1}, {"tp": row ^ 2}, {"grp": 1 - lax.axis_index("grp")}]
    for peer in peers:
        pl.semaphore_signal(barrier, inc=1, device_id=peer, device_id_type=MESH)
    pl.semaphore_wait(barrier, len(peers))


class Exchange:
    def __init__(self, count, axis, weight, joined, sems):
        self.count, self.axis, self.weight, self.joined, self.sems = (
            count, axis, weight, joined, sems
        )
        self.place, self.plane = lax.axis_index("fs"), lax.axis_index("grp")
        self.width = weight.shape[axis] // count
        self.depth = weight.shape[1 - axis]
        self.share = (self.depth if axis else self.width) // 2
        self.order = steps_by_distance(count)
        self.started = []

    def spot(self, rows, columns, row_step, column_step):
        return (
            pl.ds(pl.multiple_of(rows, row_step), self.share),
            pl.ds(pl.multiple_of(columns, column_step), self.width if self.axis else self.depth),
        )

    def leaving(self, owner, plane):
        half = plane * self.share
        if self.axis:
            return self.spot(half, owner * self.width, self.share, self.width)
        return self.spot(owner * self.width + half, 0, self.share, self.depth)

    def landing(self, source, plane):
        half = plane * self.share
        if self.axis:
            return self.spot(source * self.depth + half, 0, self.share, self.width)
        return self.spot(half, source * self.depth, self.share, self.depth)

    def copy(self, source, target, stage, step, peer):
        return pltpu.make_async_remote_copy(
            src_ref=source,
            dst_ref=target,
            send_sem=self.sems.at[stage, step],
            recv_sem=self.sems.at[stage + 1, step],
            device_id=peer,
            device_id_type=MESH,
        )

    def begin(self):
        for step in self.order:
            owner = lax.rem(self.place + step, self.count)
            moving = self.copy(
                self.weight.at[self.leaving(owner, self.plane)],
                self.joined.at[self.landing(self.place, self.plane)],
                0, step, {"fs": owner},
            )
            moving.start()
            self.started.append(moving)
        for plane in range(2):
            self.joined[self.landing(self.place, plane)] = self.weight[
                self.leaving(self.place, plane)
            ]

    def forward(self, step):
        source = lax.rem(self.place - step + self.count, self.count)
        peer = {"grp": 1 - self.plane}
        here = self.joined.at[self.landing(source, self.plane)]
        self.copy(here, here, 0, step, peer).wait_recv()
        moving = self.copy(here, here, 2, step, peer)
        moving.start()
        self.started.append(moving)

    def finish(self):
        for step in self.order:
            source = lax.rem(self.place - step + self.count, self.count)
            there = self.joined.at[self.landing(source, 1 - self.plane)]
            self.copy(there, there, 2, step, {"grp": 1 - self.plane}).wait_recv()
        for moving in self.started:
            moving.wait_send()


def joined_shape(weight, axis, count):
    shape = list(weight.shape)
    shape[axis] //= count
    shape[1 - axis] *= count
    return jax.ShapeDtypeStruct(tuple(shape), weight.dtype)


def gather_kernel(count, axes, shared, *refs):
    held, send_z, send_x, send_c, arrived, moves, extra_sems = refs[-7:]
    own_ref, gain_ref, extra_ref = refs[:3]
    number = len(axes)
    out_ref, extra_out = refs[3 + number : 5 + number]
    targets = list(refs[5 + number : -7])
    if shared:
        first = targets.pop(0)
        half = first.shape[1] // 2
        targets = [first.at[:, pl.ds(0, half)], first.at[:, pl.ds(half, half)]] + targets
    exchanges = [
        Exchange(count, axis, refs[3 + k], targets[k], moves.at[k]) for k, axis in enumerate(axes)
    ]
    place, row = lax.axis_index("fs"), lax.axis_index("tp")
    across, beside, corner = row ^ 2, row ^ 1, row ^ 3
    length, width = own_ref.shape
    greet(count, place, row)

    def copy(source, at, send_sem, peer):
        return pltpu.make_async_remote_copy(
            src_ref=source,
            dst_ref=held.at[at[0], at[1]],
            send_sem=send_sem,
            recv_sem=arrived.at[at[0], at[1]],
            device_id=peer,
            device_id_type=MESH,
        )

    started = []

    def send(source, at, send_sem, peer):
        moving = copy(source, at, send_sem, peer)
        moving.start()
        started.append(moving)

    def wait(at):
        copy(held.at[at[0], at[1]], at, arrived.at[at[0], at[1]], {"tp": beside}).wait_recv()

    order = steps_by_distance(count)
    for step in order:
        send(own_ref, (place, row), send_z.at[step], {"fs": lax.rem(place + step, count)})
    send(own_ref, (place, row), send_x.at[0], {"tp": across})
    send(own_ref, (place, row), send_c.at[0, 0], {"tp": beside})
    for step in order:
        peer = lax.rem(place + step, count)
        moving = pltpu.make_async_remote_copy(
            src_ref=extra_ref.at[0],
            dst_ref=extra_out.at[place],
            send_sem=extra_sems.at[0, step],
            recv_sem=extra_sems.at[1, step],
            device_id={"fs": peer},
            device_id_type=MESH,
        )
        moving.start()
        started.append(moving)
    extra_out[place] = extra_ref[0]
    for exchange in exchanges:
        exchange.begin()
    held[place, row] = own_ref[...]
    for step in [0] + order:
        origin = lax.rem(place - step + count, count)
        if step:
            wait((origin, row))
            block = held.at[origin, row]
            send(block, (origin, row), send_x.at[step], {"tp": across})
            send(block, (origin, row), send_c.at[0, step], {"tp": beside})
        wait((origin, across))
        send(held.at[origin, across], (origin, across), send_c.at[1, step], {"tp": beside})
    for exchange in exchanges:
        for step in order:
            exchange.forward(step)
    tile = 64
    for step in [0] + order:
        origin = lax.rem(place - step + count, count)
        wait((origin, beside))
        wait((origin, corner))

        def normalise(index, carry):
            rows = pl.ds(pl.multiple_of(index * tile, tile), tile)
            parts = [held[origin, part, rows].astype(jnp.float32) for part in range(4)]
            total = sum(jnp.sum(part * part, axis=-1, keepdims=True) for part in parts)
            inverse = lax.rsqrt(total / (4 * width) + 1e-06)
            at = pl.ds(pl.multiple_of(origin * length + index * tile, tile), tile)
            for number, part in enumerate(parts):
                columns = pl.ds(number * width, width)
                out_ref[at, columns] = (part * inverse * gain_ref[:, columns]).astype(
                    out_ref.dtype
                )
            return carry

        lax.fori_loop(0, length // tile, normalise, 0)
    for exchange in exchanges:
        exchange.finish()
    for step in order:
        there = extra_out.at[lax.rem(place - step + count, count)]
        pltpu.make_async_remote_copy(
            src_ref=there,
            dst_ref=there,
            send_sem=extra_sems.at[0, step],
            recv_sem=extra_sems.at[1, step],
            device_id={"tp": beside},
            device_id_type=MESH,
        ).wait_recv()
    for moving in started:
        moving.wait_send()


def gather_normed(rows, norm_gain, extra, weights, axes, number, shared=False):
    count = lax.axis_size("fs")
    length, width = rows.shape
    joined = [joined_shape(weight, axis, count) for weight, axis in zip(weights, axes)]
    if shared:
        deep, wide = joined.pop(0).shape
        joined[0] = jax.ShapeDtypeStruct((deep, 2 * wide), rows.dtype)
    vmem = pl.BlockSpec(memory_space=pltpu.VMEM)
    dma = pltpu.SemaphoreType.DMA
    return pl.pallas_call(
        functools.partial(gather_kernel, count, axes, shared),
        out_shape=[
            jax.ShapeDtypeStruct((count * length, 4 * width), rows.dtype),
            jax.ShapeDtypeStruct((count, 1, length), extra.dtype),
        ]
        + joined,
        in_specs=[vmem] * (3 + len(axes)),
        out_specs=[vmem] * (2 + len(joined)),
        scratch_shapes=[
            pltpu.VMEM((count, 4, length, width), rows.dtype),
            dma((count,)),
            dma((count,)),
            dma((2, count)),
            dma((count, 4)),
            dma((len(axes), 4, count)),
            dma((2, count)),
        ],
        compiler_params=pltpu.CompilerParams(
            collective_id=number, has_side_effects=True, vmem_limit_bytes=32 * 2**20
        ),
        cost_estimate=pl.CostEstimate(flops=10**9, bytes_accessed=10**8, transcendentals=0),
    )(rows, norm_gain.reshape(1, -1), extra.reshape(1, 1, -1), *weights)


def scatter_kernel(count, axes, *refs):
    number = len(axes)
    terms_ref, base_ref = refs[:2]
    out_ref = refs[2 + number]
    from_core, to_x, from_x, to_z, from_z, send_c, recv_c, send_x, recv_x, send_z, recv_z = refs[
        3 + 2 * number : 14 + 2 * number
    ]
    exchanges = [
        Exchange(count, axis, refs[2 + k], refs[3 + number + k], refs[-1].at[k])
        for k, axis in enumerate(axes)
    ]
    place, row = lax.axis_index("fs"), lax.axis_index("tp")
    across, beside, corner = row ^ 2, row ^ 1, row ^ 3
    length, width = base_ref.shape
    greet(count, place, row)
    started = []

    def copy(source, target, send_sem, recv_sem, peer):
        return pltpu.make_async_remote_copy(
            src_ref=source,
            dst_ref=target,
            send_sem=send_sem,
            recv_sem=recv_sem,
            device_id=peer,
            device_id_type=MESH,
        )

    def send(*given):
        moving = copy(*given)
        moving.start()
        started.append(moving)

    def block(step, part):
        owner = lax.rem(place + step, count)
        return (
            pl.ds(pl.multiple_of(owner * length, length), length),
            pl.ds(pl.multiple_of(part * width, width), width),
        )

    def core_copy(step, side):
        part = corner if side else beside
        return (
            terms_ref.at[block(step, part)],
            from_core.at[side, step],
            send_c.at[side, step],
            recv_c.at[side, step],
            {"tp": beside},
        )

    def x_copy(step):
        return (to_x.at[step], from_x.at[step], send_x.at[step], recv_x.at[step], {"tp": across})

    def z_copy(step):
        peer = {"fs": lax.rem(place + step, count)}
        return (to_z.at[step], from_z.at[step], send_z.at[step], recv_z.at[step], peer)

    order = steps_by_distance(count)[::-1] + [0]
    for step in order:
        for side in (1, 0):
            send(*core_copy(step, side))
    wide = jnp.float32
    for exchange in exchanges:
        exchange.begin()
    for step in order:
        copy(*core_copy(step, 1)).wait_recv()
        mine = terms_ref[block(step, across)].astype(wide)
        to_x[step] = (mine + from_core[1, step].astype(wide)).astype(to_x.dtype)
        send(*x_copy(step))
    total = base_ref[...].astype(wide)
    summed = None
    for turn, step in enumerate(order):
        if turn:
            for exchange in exchanges:
                exchange.forward(exchange.order[turn - 1])
        copy(*core_copy(step, 0)).wait_recv()
        copy(*x_copy(step)).wait_recv()
        mine = terms_ref[block(step, row)].astype(wide) + from_core[0, step].astype(wide)
        mine = mine + from_x[step].astype(wide)
        if step:
            to_z[step] = mine.astype(to_z.dtype)
            send(*z_copy(step))
        else:
            summed = mine
    for step in order[:-1]:
        copy(*z_copy(step)).wait_recv()
        summed = summed + from_z[step].astype(wide)
    out_ref[...] = (total + summed).astype(out_ref.dtype)
    for exchange in exchanges:
        exchange.finish()
    for moving in started:
        moving.wait_send()


def scatter_added(terms, base, weights, axes, number):
    count = lax.axis_size("fs")
    vmem = pl.BlockSpec(memory_space=pltpu.VMEM)
    dma = pltpu.SemaphoreType.DMA
    blocks = pltpu.VMEM((count,) + base.shape, base.dtype)
    return pl.pallas_call(
        functools.partial(scatter_kernel, count, axes),
        out_shape=[jax.ShapeDtypeStruct(base.shape, base.dtype)]
        + [joined_shape(weight, axis, count) for weight, axis in zip(weights, axes)],
        in_specs=[vmem] * (2 + len(axes)),
        out_specs=[vmem] * (1 + len(axes)),
        scratch_shapes=[pltpu.VMEM((2, count) + base.shape, base.dtype)]
        + [blocks] * 4
        + [dma((2, count))] * 2
        + [dma((count,))] * 4
        + [dma((len(axes), 4, count)) for _ in axes[:1]],
        compiler_params=pltpu.CompilerParams(
            collective_id=number, has_side_effects=True, vmem_limit_bytes=24 * 2**20
        ),
        cost_estimate=pl.CostEstimate(flops=10**9, bytes_accessed=10**8, transcendentals=0),
    )(terms, base, *weights)


def recurrence_kernel(
    gate_ref, recur_ref, taps_ref, decay_map_ref, input_map_ref, rate_ref, extra_ref, out_ref
):
    wide = jnp.float32
    recur = recur_ref[...].astype(jnp.bfloat16).astype(wide)
    length = recur.shape[0]
    position = lax.broadcasted_iota(jnp.int32, recur.shape, 0)
    taps = taps_ref.shape[0]
    conv = recur * taps_ref[taps - 1 : taps].astype(wide)
    for tap in range(taps - 1):
        back = taps - 1 - tap
        earlier = jnp.where(position >= back, pltpu.roll(recur, back, 0), 0.0)
        conv = conv + earlier * taps_ref[tap : tap + 1].astype(wide)
    conv_rows = conv.astype(jnp.bfloat16)
    recur_gate = jax.nn.sigmoid(
        jnp.dot(conv_rows, decay_map_ref[0], preferred_element_type=wide)
    )
    input_rate = jax.nn.sigmoid(
        jnp.dot(conv_rows, input_map_ref[0], preferred_element_type=wide)
    )
    log_decay = rate_ref[...] * recur_gate + extra_ref[...]
    decay = jnp.exp(log_decay)
    spread = -jnp.tanh(log_decay) * (decay * decay + 1.0)
    drive = jnp.sqrt(spread) * input_rate * conv_rows.astype(wide)
    back = 1
    while back < length:
        inside = position >= back
        drive = drive + decay * jnp.where(inside, pltpu.roll(drive, back, 0), 0.0)
        if back * 2 < length:
            decay = decay * jnp.where(inside, pltpu.roll(decay, back, 0), 1.0)
        back *= 2
    gate_rows = jax.nn.gelu(gate_ref[...]).astype(jnp.bfloat16)
    out_ref[...] = (drive * gate_rows.astype(wide)).astype(out_ref.dtype)


def recurrence(both, taps, decay_map, input_map, rate, extra, count):
    blocks, size, _ = decay_map.shape
    length = both.shape[0] // count
    return pl.pallas_call(
        recurrence_kernel,
        grid=(count, blocks),
        out_shape=jax.ShapeDtypeStruct((count * length, blocks * size), jnp.bfloat16),
        in_specs=[
            pl.BlockSpec((length, size), lambda s, n: (s, n)),
            pl.BlockSpec((length, size), lambda s, n: (s, n + blocks)),
            pl.BlockSpec((taps.shape[0], size), lambda s, n: (0, n)),
            pl.BlockSpec((1, size, size), lambda s, n: (n, 0, 0)),
            pl.BlockSpec((1, size, size), lambda s, n: (n, 0, 0)),
            pl.BlockSpec((1, size), lambda s, n: (0, n)),
            pl.BlockSpec((length, 1), lambda s, n: (s, 0)),
        ],
        out_specs=pl.BlockSpec((length, size), lambda s, n: (s, n)),
        compiler_params=pltpu.CompilerParams(vmem_limit_bytes=24 * 2**20),
        cost_estimate=pl.CostEstimate(flops=10**8, bytes_accessed=10**7, transcendentals=10**6),
    )(both, both, taps, decay_map, input_map, rate.reshape(1, -1), extra.reshape(-1, 1))


def per_device_owned(
    tokens,
    recurrent_norm_gain,
    feedforward_norm_gain,
    gate_projection_weight,
    recurrent_projection_weight,
    convolution_kernel,
    decay_gate_matrix,
    input_gate_matrix,
    base_decay_logit,
    extra_log_decay,
    output_projection_weight,
    up_projection_weight,
    down_projection_weight,
):
    count, mine = lax.axis_size("fs"), lax.axis_index("fs")

    def own(value, axis):
        width = value.shape[axis] // count
        return lax.dynamic_slice_in_dim(value, mine * width, width, axis)

    normed, extra, both_weight, out_weight = gather_normed(
        tokens,
        recurrent_norm_gain,
        extra_log_decay,
        (gate_projection_weight, recurrent_projection_weight, output_projection_weight),
        (1, 1, 0),
        1,
        shared=True,
    )
    mixed = recurrence(
        jnp.dot(normed, both_weight, preferred_element_type=jnp.float32),
        own(convolution_kernel, 1),
        own(decay_gate_matrix, 0),
        own(input_gate_matrix, 0),
        -8.0 * jax.nn.softplus(-own(base_decay_logit, 0)),
        extra,
        count,
    )
    partials = jnp.dot(mixed, out_weight, preferred_element_type=jnp.float32)
    residual, up_weight = scatter_added(
        partials.astype(jnp.bfloat16), tokens, (up_projection_weight,), (1,), 2
    )
    channel_in, _, down_weight = gather_normed(
        residual, feedforward_norm_gain, extra_log_decay, (down_projection_weight,), (0,), 3
    )
    positive = jnp.maximum(
        jnp.dot(channel_in, up_weight, preferred_element_type=jnp.float32), 0.0
    )
    squared = (positive * positive).astype(jnp.bfloat16)
    down_terms = jnp.dot(squared, down_weight, preferred_element_type=jnp.float32)
    return scatter_added(down_terms.astype(jnp.bfloat16), residual, (), (), 4)[0]


def solution(mesh):
    placed = (
        P(("grp", "fs"), "tp"),
        P(),
        P(),
        P("fs", "tp"),
        P("fs", "tp"),
        P(None, "tp"),
        P("tp", None, None),
        P("tp", None, None),
        P("tp"),
        P(("grp", "fs")),
        P("tp", "fs"),
        P("fs", "tp"),
        P("tp", "fs"),
    )
    owners = mesh.shape["fs"] * mesh.shape["tp"]
    fitting = mesh.shape["tp"] == 4 and mesh.shape["grp"] == 2

    def run(*arrays):
        owned = fitting and arrays[6].shape[0] % owners == 0
        body = per_device_owned if owned else per_device
        return jax.shard_map(
            body, mesh=mesh, in_specs=placed, out_specs=P(("grp", "fs"), "tp"), check_vma=False
        )(*arrays)

    return run
```
